32 devices in a mesh: sp: 16 (over z, y, x), tp: 2 (over core).
Axes of the slice: x: 2, y: 2, z: 4, core: 2. Of those that a mesh axis runs over, the one named last changes fastest.
Arguments:
- residual: bfloat16 [4096, 2048], P(('sp', 'tp')), may hold values from -6 to 6
- pool_input: bfloat16 [4096, 1024], P('sp', 'tp'), may hold values from -6 to 6
- group_maps: bfloat16 [8, 128, 128], replicated, may hold values from -0.5 to 0.5
- pool_scale: float32 [1024], replicated, may hold values from 0.1 to 1.9
- out_proj: bfloat16 [1024, 2048], replicated, may hold values from -0.1875 to 0.1875
- norm_gain: float32 [2048], replicated, may hold values from 0.1 to 1.9
- shared_gate: bfloat16 [2048, 512], replicated, may hold values from -0.125 to 0.125
- shared_up: bfloat16 [2048, 512], replicated, may hold values from -0.125 to 0.125
- shared_down: bfloat16 [512, 2048], replicated, may hold values from -0.25 to 0.25
- expert_gate: bfloat16 [32, 2048, 512], P(('sp', 'tp')), may hold values from -0.125 to 0.125
- expert_up: bfloat16 [32, 2048, 512], P(('sp', 'tp')), may hold values from -0.125 to 0.125
- expert_down: bfloat16 [32, 512, 2048], P(('sp', 'tp')), may hold values from -0.25 to 0.25
- expert_ids: int32 [4096, 4], P(('sp', 'tp')), may hold values from 0 to 31, all different within a row; in each aligned block of 128 rows (0 to 127, 128 to 255, ...) at most 24 rows name the same one
- route_score: float32 [4096, 4], P(('sp', 'tp')), may hold values from 0.05 to 1
Outputs:
- output: bfloat16 [4096, 2048], P(('sp', 'tp'))
The draws below stay inside these ranges and needn't reach their ends.
Inputs may be any that keep to these rules, and one draw needn't show every extreme that they name: `expert_ids`: each row names 4 different experts; among the 128 rows of one device no expert is named more than 24 times, and in some devices' rows one expert is named exactly 24 times.
All inputs are finite; a program needn't handle non-finite values.
Results may differ from the reference program's by a relative error of at most 0.015.
Values may be sent and summed in bfloat16 or wider, within the bound.
No kernel may reach another device: no remote copies, remote signals or barrier semaphores. Data moves between devices by JAX's collectives and lax.ppermute only.
A program may use at most 128 MiB of HBM per device.

```python
import math
import jax
import jax.numpy as jnp
import numpy as np
from jax import lax

D = 2048
POOL_GROUPS = 8
GROUP_WIDTH = 128
EXPERT_HIDDEN = 512
SHARED_HIDDEN = 512
TOPK = 4
TOK_DEV = 128
TOKENS = 4096
POOL = 1024
EXPERTS = 32
CAP = 24


def shard_levels(own_key, shape, shards, least, high):
    def one(position, parts):
        draws = jax.random.uniform(jax.random.fold_in(jax.random.fold_in(own_key, 6), position), (parts,), jnp.float32, least / len(shards), high / len(shards))
        return jnp.repeat(jnp.exp(draws), shape[position] // parts).reshape((-1,) + (1,) * (len(shape) - position - 1))

    gain = one(*shards[0])
    for cut in shards[1:]:
        gain = gain * one(*cut)
    return gain


def shared_out(stream_key, own, number, rows, amount, top, reach, lean):
    ranking = jax.random.permutation(stream_key, amount)
    heavy_load, common = portions_of(amount, rows * top, reach, lean, True), portions_of(amount, rows * top, reach, lean, False)
    places = jnp.arange(amount)

    def named(tallies, rotation):
        used = int((tallies > 0).sum())
        fixed = max(1, used // 4)
        moved = fixed + (places - fixed + rotation * (used - fixed)) % max(1, amount - fixed)
        return jnp.zeros((amount,), jnp.int32).at[ranking[jnp.where(places < fixed, places, moved)]].set(jnp.asarray(tallies, jnp.int32))

    tallies = jnp.where(number % 4 == 0, named(heavy_load, number // 4), named(common, number - number // 4 - 1))
    mixed = jax.random.permutation(jax.random.fold_in(own, 3), amount)
    source_of, taker = mixed[0:amount // 2 * 2:2], mixed[1:amount // 2 * 2:2]
    slack = jnp.minimum(tallies[source_of] - 1, reach - tallies[taker]) // 2
    slack = jnp.where((source_of == ranking[0]) | (taker == ranking[0]) | (tallies[taker] == 0), 0, jnp.maximum(slack, 0))
    moved = jax.random.randint(jax.random.fold_in(own, 4), (amount // 2,), 0, 1 << 20) % (slack + 1)
    tallies = tallies.at[source_of].add(-moved).at[taker].add(moved)
    items = jnp.searchsorted(jnp.cumsum(tallies), jnp.arange(rows * top), side="right").astype(jnp.int32)
    table = items.reshape(top, rows).T
    table = table[jax.random.permutation(jax.random.fold_in(own, 1), rows)]
    rotation = jax.random.randint(jax.random.fold_in(own, 2), (rows, 1), 0, top)
    return jnp.take_along_axis(table, (jnp.arange(top)[None, :] + rotation) % top, axis=1)


def portions_of(count, total, bound, slope, full):
    loads = [(1 << 20) // math.isqrt(rank ** slope) + 1 for rank in range(1, count + 1)]
    largest = bound if full else min(bound, max(-(-total // count), total * loads[0] // sum(loads)))
    least = 1 if total - largest >= count - 1 else 0
    given, rest = [largest] + [least] * (count - 1), total - largest - least * (count - 1)
    while rest > 0:
        free = [i for i in range(1, count) if given[i] < largest] or [i for i in range(1, count) if given[i] < bound]
        mass, budget = sum([loads[i] for i in free]), rest
        for i in free:
            more = min(bound - given[i], max(1, budget * loads[i] // mass), rest)
            given[i] = given[i] + more
            rest = rest - more
    return np.array(given)


def bell_draw(stream_key, shape, spread, bound, shards=(), kind=jnp.bfloat16):
    drawn = spread * jax.random.normal(stream_key, shape, jnp.float32)
    if shards:
        drawn = drawn * shard_levels(stream_key, shape, shards, -0.22, 0.18)
    return jnp.clip(drawn, -bound, bound).astype(kind)


def setup_inputs(seed: int = 0) -> dict:
    keys = jax.random.split(jax.random.key(seed), 15)
    residual = bell_draw(keys[0], (TOKENS, D), 1.0, 6.0, ((0, 32),))
    pool_input = bell_draw(keys[1], (TOKENS, POOL), 1.0, 6.0, ((0, 16), (1, 2)))
    group_maps = bell_draw(keys[2], (POOL_GROUPS, GROUP_WIDTH, GROUP_WIDTH), GROUP_WIDTH ** -0.5, 0.5)
    pool_scale = jnp.clip(1.0 + 0.18 * jax.random.normal(keys[3], (POOL,), jnp.float32), 0.1, 1.9)
    out_proj = bell_draw(keys[4], (POOL, D), POOL ** -0.5, 0.1875)
    norm_gain = jnp.clip(1.0 + 0.18 * jax.random.normal(keys[5], (D,), jnp.float32), 0.1, 1.9)
    shared_gate = bell_draw(keys[6], (D, SHARED_HIDDEN), D ** -0.5, 0.125)
    shared_up = bell_draw(keys[7], (D, SHARED_HIDDEN), D ** -0.5, 0.125)
    shared_down = bell_draw(keys[8], (SHARED_HIDDEN, D), SHARED_HIDDEN ** -0.5, 0.25)
    expert_gate = bell_draw(keys[9], (EXPERTS, D, EXPERT_HIDDEN), D ** -0.5, 0.125, ((0, 32),))
    expert_up = bell_draw(keys[10], (EXPERTS, D, EXPERT_HIDDEN), D ** -0.5, 0.125, ((0, 32),))
    expert_down = bell_draw(keys[11], (EXPERTS, EXPERT_HIDDEN, D), EXPERT_HIDDEN ** -0.5, 0.25, ((0, 32),))
    expert_ids_keys = jax.random.split(jax.random.fold_in(keys[12], 1), TOKENS // TOK_DEV)
    expert_ids_turns = jax.random.permutation(jax.random.fold_in(keys[12], 3), TOKENS // TOK_DEV)
    expert_ids = jax.vmap(lambda own, number: shared_out(jax.random.fold_in(keys[12], 2), own, number, TOK_DEV, EXPERTS, TOPK, CAP, 2))(expert_ids_keys, expert_ids_turns).reshape((TOKENS, TOPK))
    route_score = jnp.clip(0.05 + 0.95 * jax.random.uniform(keys[13], (TOKENS, TOPK), jnp.float32) ** shard_levels(keys[13], (TOKENS, TOPK), ((0, 32),), -0.2, 0.2), 0.05, 1.0)
    return dict(residual=residual, pool_input=pool_input, group_maps=group_maps, pool_scale=pool_scale, out_proj=out_proj, norm_gain=norm_gain, shared_gate=shared_gate, shared_up=shared_up, shared_down=shared_down, expert_gate=expert_gate, expert_up=expert_up, expert_down=expert_down, expert_ids=expert_ids, route_score=route_score)


windows = (2, 4, 8, 16)
epsilon = 1e-06
routed_scale = 2.5

def swiglu(row_block, w_gate, w_up, w_down):
    gate_part = jnp.dot(row_block, w_gate, preferred_element_type=jnp.float32)
    up_part = jnp.dot(row_block, w_up, preferred_element_type=jnp.float32)
    hidden = (jax.nn.silu(gate_part) * up_part).astype(jnp.bfloat16)
    return jnp.dot(hidden, w_down, preferred_element_type=jnp.float32)

def reference(residual, pool_input, group_maps, pool_scale, out_proj, norm_gain, shared_gate, shared_up, shared_down, expert_gate, expert_up, expert_down, expert_ids, route_score):
    length = pool_input.shape[0]
    groups = group_maps.shape[0]
    group_width = group_maps.shape[1]
    input_values = pool_input.astype(jnp.float32).reshape(length, groups, group_width)
    places = jnp.arange(length, dtype=jnp.int32)
    pooled = []
    for group_index in range(groups):
        window_span = windows[group_index % 4]
        group_column = input_values[:, group_index]
        padded = jnp.pad(group_column, ((window_span - 1, 0), (0, 0)))
        running_sum = padded[window_span - 1:]
        for offset_shift in range(1, window_span):
            running_sum = running_sum + padded[window_span - 1 - offset_shift:window_span - 1 - offset_shift + length]
        divisor = jnp.minimum(places + 1, window_span).astype(jnp.float32)[:, None]
        pooled.append(running_sum / divisor)
    pooled = jnp.stack(pooled, axis=1)
    contrast = (pooled - input_values).astype(jnp.bfloat16)
    mapped = jnp.einsum('sgc,gcd->sgd', contrast.astype(jnp.float32), group_maps.astype(jnp.float32))
    mixed_rows = (mapped.reshape(length, groups * group_width) * pool_scale).astype(jnp.bfloat16)
    projected = jnp.dot(mixed_rows, out_proj, preferred_element_type=jnp.float32)
    settled = (residual.astype(jnp.float32) + projected).astype(jnp.bfloat16)
    settled_wide = settled.astype(jnp.float32)
    inverse_rms = lax.rsqrt(lax.optimization_barrier(jnp.mean(settled_wide * settled_wide, axis=-1, keepdims=True)) + epsilon)
    normed = (settled_wide * inverse_rms * norm_gain).astype(jnp.bfloat16)
    shared = swiglu(normed, shared_gate, shared_up, shared_down)
    weights = route_score / lax.optimization_barrier(jnp.sum(route_score, axis=-1, keepdims=True)) * routed_scale
    experts = expert_gate.shape[0]
    top_count = expert_ids.shape[1]
    assigned = length * top_count
    flat_ids = expert_ids.reshape(assigned).astype(jnp.int32)
    sort_order = jnp.argsort(flat_ids, stable=True).astype(jnp.int32)
    sorted_ids = flat_ids[sort_order]
    counts = jnp.bincount(flat_ids, length=experts).astype(jnp.int32)
    starts = jnp.cumsum(counts).astype(jnp.int32) - counts
    expert_depth = EXPERTS * CAP
    slot_rank = jnp.arange(assigned, dtype=jnp.int32) - starts[sorted_ids]
    slot_index = sorted_ids * expert_depth + slot_rank
    slot_token = jnp.zeros((experts * expert_depth,), jnp.int32).at[slot_index].set(sort_order // top_count)
    slot_weight = jnp.zeros((experts * expert_depth,), jnp.float32).at[slot_index].set(weights.reshape(assigned)[sort_order])

    def one_expert(routed, inputs):
        token_index, slot_factor, w_gate, w_up, w_down = inputs
        expert_rows = swiglu(normed[token_index], w_gate, w_up, w_down).astype(jnp.bfloat16)
        return (routed.at[token_index].add(slot_factor[:, None] * expert_rows.astype(jnp.float32)), None)
    routed, _ = lax.scan(one_expert, jnp.zeros((length, D), jnp.float32), (slot_token.reshape(experts, expert_depth), slot_weight.reshape(experts, expert_depth), expert_gate, expert_up, expert_down))
    return (settled_wide + shared + routed).astype(jnp.bfloat16)
```

```python
import functools

import jax
import jax.numpy as jnp
from jax import lax
from jax.experimental import pallas as pl
from jax.experimental.pallas import tpu as pltpu
from jax.sharding import PartitionSpec as P

windows = (2, 4, 8, 16)
epsilon = 1e-06
routed_scale = 2.5
f32 = jnp.float32
bf16 = jnp.bfloat16
halo = max(windows)
MIB = 1 << 20


vmem = pl.BlockSpec(memory_space=pltpu.VMEM)
smem = pl.BlockSpec(memory_space=pltpu.SMEM)


def call(body, outs, n_in, name, flops, nbytes, limit, scalars=0):
    return pl.pallas_call(
        body,
        out_shape=outs,
        in_specs=[smem] * scalars + [vmem] * n_in,
        out_specs=jax.tree.map(lambda _: vmem, outs),
        name=name,
        cost_estimate=pl.CostEstimate(flops=flops, bytes_accessed=nbytes, transcendentals=0),
        compiler_params=pltpu.CompilerParams(vmem_limit_bytes=limit),
    )


def dot(a, b):
    return jnp.dot(a, b, preferred_element_type=f32)


def silu_mul(gate, up):
    return gate / (1.0 + jnp.exp(-gate)) * up


def mixer_body(parts, where, *refs):
    mains, halos = refs[:parts], refs[parts : 2 * parts]
    residual, maps, scale, proj, gain, settled_ref, normed_ref, mixed_ref = refs[2 * parts :]
    rows, channels = mains[0].shape
    width = maps.shape[1]
    groups_here = channels // width
    place = where[0] * rows + lax.broadcasted_iota(jnp.int32, (rows, width), 0)
    for j in range(parts):
        part = lax.rem(where[1] + parts - j, parts)
        for g in range(groups_here):
            cols = slice(g * width, (g + 1) * width)
            here = mains[j][:, cols].astype(f32)
            total = jnp.concatenate([halos[j][:, cols].astype(f32), here], axis=0)
            span = 1
            while span < windows[g % 4]:
                total = total + pltpu.roll(total, span, 0)
                span *= 2
            pooled = total[halo:] / jnp.minimum(place + 1, span).astype(f32)
            contrast = (pooled - here).astype(bf16)
            group = part * groups_here + g
            mapped = dot(contrast, maps[group]) * scale[pl.ds(group, 1), :]
            at = pl.multiple_of(group * width, width)
            mixed_ref[:, pl.ds(at, width)] = mapped.astype(bf16)
    model = residual.shape[1]
    step = min(model, 512)
    squares = jnp.zeros((rows, 1), f32)
    for c in range(0, model, step):
        wide = residual[:, c : c + step].astype(f32) + dot(mixed_ref[...], proj[:, c : c + step])
        wide = wide.astype(bf16)
        settled_ref[:, c : c + step] = wide
        wide = wide.astype(f32)
        squares = squares + jnp.sum(wide * wide, axis=1, keepdims=True)
    inverse = lax.rsqrt(squares / model + epsilon)
    for c in range(0, model, step):
        wide = settled_ref[:, c : c + step].astype(f32)
        normed_ref[:, c : c + step] = (wide * inverse * gain[:, c : c + step]).astype(bf16)


def mixer(parts, where, mains, halos, residual, maps, scale, proj, gain):
    rows, model = residual.shape
    out = jax.ShapeDtypeStruct((rows, model), bf16)
    return pl.pallas_call(
        functools.partial(mixer_body, parts),
        out_shape=(out, out),
        in_specs=[smem] + [vmem] * (2 * parts + 5),
        out_specs=(vmem, vmem),
        scratch_shapes=[pltpu.VMEM((rows, proj.shape[0]), bf16)],
        name="mixer",
        cost_estimate=pl.CostEstimate(
            flops=2 * rows * proj.size, bytes_accessed=2 * proj.size, transcendentals=0
        ),
        compiler_params=pltpu.CompilerParams(vmem_limit_bytes=24 * MIB),
    )(where, *mains, *halos, residual, maps, scale, proj, gain)


def shared_body(normed, settled, gate, up, down, base_ref):
    hidden = silu_mul(dot(normed[...], gate[...]), dot(normed[...], up[...])).astype(bf16)
    model = base_ref.shape[1]
    step = min(model, 512)
    for c in range(0, model, step):
        base_ref[:, c : c + step] = settled[:, c : c + step].astype(f32) + dot(
            hidden, down[:, c : c + step]
        )


def pack_body(slots, top, where, meta, rows_ref, *outs):
    count = len(outs) - 2
    high_ref, low_ref = outs[count:]
    tokens = rows_ref.shape[0]
    first, mine = where[0], where[1]
    expert = first + (mine ^ lax.broadcasted_iota(jnp.int32, (count, tokens), 0))
    expert = expert.astype(f32)
    scores = meta[top : 2 * top, :]
    shares = scores / jnp.sum(scores, axis=0, keepdims=True) * routed_scale
    named = jnp.zeros((count, tokens), f32)
    weight = jnp.zeros((count, tokens), f32)
    for k in range(top):
        hit = meta[k : k + 1, :] == expert
        named = jnp.where(hit, 1.0, named)
        weight = jnp.where(hit, shares[k : k + 1, :], weight)
    earlier = lax.broadcasted_iota(jnp.int32, (tokens, tokens), 0) < lax.broadcasted_iota(
        jnp.int32, (tokens, tokens), 1
    )
    position = dot(named.astype(bf16), earlier.astype(f32).astype(bf16))
    position = jnp.where(named > 0, position, -1.0)
    slot = lax.broadcasted_iota(jnp.int32, (slots, tokens), 0).astype(f32)
    picks = [jnp.where(position[j : j + 1, :] == slot, 1.0, 0.0) for j in range(count)]
    factors = jnp.concatenate([picks[j] * weight[j : j + 1, :] for j in range(count)], axis=0)
    picks = jnp.concatenate(picks, axis=0).astype(bf16)
    high = factors.astype(bf16)
    high_ref[...] = high
    low_ref[...] = (factors - high.astype(f32)).astype(bf16)
    model = rows_ref.shape[1]
    step = min(model, 512)
    for c in range(0, model, step):
        chosen = dot(picks, rows_ref[:, c : c + step])
        for j in range(count):
            outs[j][:, c : c + step] = chosen[j * slots : (j + 1) * slots].astype(bf16)


def pack(count, slots, where, meta, rows):
    tokens, model = rows.shape
    piece = jax.ShapeDtypeStruct((slots, model), bf16)
    factor = jax.ShapeDtypeStruct((count * slots, tokens), bf16)
    out = call(
        functools.partial(pack_body, slots, meta.shape[0] // 2),
        (piece,) * count + (factor,) * 2,
        2,
        "pack",
        2 * count * slots * tokens * model,
        4 * rows.size,
        16 * MIB,
        1,
    )(where, meta, rows)
    return out[:count], out[count:]


def gathered(refs):
    return jnp.concatenate([r[...].astype(f32) for r in refs], axis=0).astype(bf16)


def expert_body(count, *refs):
    pieces = refs[:count]
    gate, up, down = refs[count : count + 3]
    outs = refs[count + 3 : 2 * count + 3]
    held = refs[2 * count + 3]
    slots, model = pieces[0].shape
    held[...] = gathered(pieces)
    hidden = silu_mul(dot(held[...], gate[0]), dot(held[...], up[0])).astype(bf16)
    step = min(model, 512)
    for c in range(0, model, step):
        result = dot(hidden, down[0, :, c : c + step])
        for j in range(count):
            outs[j][:, c : c + step] = result[j * slots : (j + 1) * slots].astype(bf16)


def expert(pieces, gate, up, down):
    count = len(pieces)
    slots, model = pieces[0].shape
    piece = jax.ShapeDtypeStruct((slots, model), bf16)
    return pl.pallas_call(
        functools.partial(expert_body, count),
        out_shape=(piece,) * count,
        in_specs=[vmem] * (count + 3),
        out_specs=(vmem,) * count,
        scratch_shapes=[pltpu.VMEM((count * slots, model), bf16)],
        name="expert",
        cost_estimate=pl.CostEstimate(
            flops=6 * count * slots * gate.size, bytes_accessed=6 * gate.size, transcendentals=0
        ),
        compiler_params=pltpu.CompilerParams(vmem_limit_bytes=24 * MIB),
    )(*pieces, gate, up, down)


def weighted(high, low, rows):
    dims = (((0,), (0,)), ((), ()))
    return lax.dot_general(high, rows, dims, preferred_element_type=f32) + lax.dot_general(
        low, rows, dims, preferred_element_type=f32
    )


def combine_body(count, *refs):
    pieces, (high, low, out_ref) = refs[:count], refs[count:]
    model = out_ref.shape[1]
    step = min(model, 512)
    for c in range(0, model, step):
        rows = gathered([r.at[:, c : c + step] for r in pieces])
        out_ref[:, c : c + step] = weighted(high[...], low[...], rows).astype(bf16)


def combine(pieces, factors):
    count = len(pieces)
    slots, model = pieces[0].shape
    tokens = factors[0].shape[1]
    return call(
        functools.partial(combine_body, count),
        jax.ShapeDtypeStruct((tokens, model), bf16),
        count + 2,
        "combine",
        4 * count * slots * tokens * model,
        2 * count * slots * model,
        16 * MIB,
    )(*pieces, *factors)


def final_body(count, extra, *refs):
    pieces = refs[:count]
    high, low, base = refs[count : count + 3]
    partials = refs[count + 3 : count + 3 + extra]
    out_ref = refs[count + 3 + extra]
    model = out_ref.shape[1]
    step = min(model, 512)
    for c in range(0, model, step):
        cols = slice(c, c + step)
        rows = gathered([r.at[:, cols] for r in pieces])
        total = base[:, cols] + weighted(high[...], low[...], rows)
        for p in partials:
            total = total + p[:, cols].astype(f32)
        out_ref[:, cols] = total.astype(bf16)


def final(pieces, factors, base, partials):
    count = len(pieces)
    return call(
        functools.partial(final_body, count, len(partials)),
        jax.ShapeDtypeStruct(base.shape, bf16),
        count + 3 + len(partials),
        "final",
        4 * count * pieces[0].shape[0] * base.size,
        4 * base.size,
        16 * MIB,
    )(*pieces, *factors, base, *partials)


def on_device(
    residual,
    pool_input,
    group_maps,
    pool_scale,
    out_proj,
    norm_gain,
    shared_gate,
    shared_up,
    shared_down,
    expert_gate,
    expert_up,
    expert_down,
    expert_ids,
    route_score,
):
    axes = ("sp", "tp")
    size_sp, size_tp = lax.axis_size("sp"), lax.axis_size("tp")
    devices = size_sp * size_tp
    me = lax.axis_index(axes)
    my_tp = lax.axis_index("tp")
    tokens, model = residual.shape
    block_rows, channels = pool_input.shape
    top = expert_ids.shape[1]
    capacity = 3 * tokens * top // (2 * devices)
    slots = -(-capacity // 8) * 8
    planes = 1
    while size_sp % (2 * planes) == 0 and capacity * devices >= 2 * planes * tokens:
        planes *= 2
    size_plane = devices // planes

    def move(x, target):
        pairs = [(i, target(i)) for i in range(devices)]
        return lax.ppermute(x, axes, [p for p in pairs if p[1] is not None])

    def along(by):
        return lambda i: (i + by * size_plane) % devices

    def inside(j):
        return lambda i: i // size_plane * size_plane + (i % size_plane ^ j)

    mains, halos = [], []
    for j in range(size_tp):
        to = lax.rem(my_tp + j, size_tp)
        main = lax.dynamic_slice_in_dim(pool_input, to * tokens, tokens, 0)
        start = lax.rem(to * tokens + block_rows - halo, block_rows)
        tail = lax.dynamic_slice_in_dim(pool_input, start, halo, 0)

        def main_to(i, j=j):
            return i // size_tp * size_tp + (i + j) % size_tp

        def tail_to(i, j=j):
            t = main_to(i, j)
            if t % size_tp:
                return t
            return t + size_tp if t + size_tp < devices else None

        mains.append(move(main, main_to) if j else main)
        halos.append(move(tail, tail_to))
    meta = jnp.concatenate([expert_ids.astype(f32).T, route_score.T], axis=0)
    metas = [meta] + [move(meta, along(k)) for k in range(1, planes)]

    where = jnp.stack([me, my_tp]).astype(jnp.int32)
    settled, normed = mixer(
        size_tp,
        where,
        mains,
        halos,
        residual,
        group_maps,
        pool_scale.reshape(-1, group_maps.shape[1]),
        out_proj,
        norm_gain.reshape(1, -1),
    )
    base = call(
        shared_body,
        jax.ShapeDtypeStruct((tokens, model), f32),
        5,
        "shared",
        6 * tokens * shared_gate.size,
        6 * shared_gate.size,
        24 * MIB,
    )(normed, settled, shared_gate, shared_up, shared_down)

    mine = lax.rem(me, size_plane)
    spot = jnp.stack([me - mine, mine]).astype(jnp.int32)
    block = normed
    partials = []
    for k in range(planes):
        if k:
            block = move(block, along(1))
        pieces, factors = pack(size_plane, slots, spot, metas[k], block)
        pieces = [move(p, inside(j)) if j else p for j, p in enumerate(pieces)]
        results = expert(pieces, expert_gate, expert_up, expert_down)
        results = [move(r, inside(j)) if j else r for j, r in enumerate(results)]
        if k:
            partials.append(move(combine(results, factors), along(-k)))
        else:
            own = results, factors
    return final(*own, base, partials)


def solution(mesh):
    lines = P(("sp", "tp"), None)
    stacked = P(("sp", "tp"), None, None)
    in_specs = (
        (lines, P("sp", "tp")) + (P(),) * 7 + (stacked,) * 3 + (lines, lines)
    )
    return jax.shard_map(
        on_device, mesh=mesh, in_specs=in_specs, out_specs=lines, check_vma=False
    )
```

```python
import functools

import jax
import jax.numpy as jnp
from jax import lax
from jax.experimental import pallas as pl
from jax.experimental.pallas import tpu as pltpu
from jax.sharding import PartitionSpec as P


windows = (2, 4, 8, 16)
epsilon = 1e-06
routed_scale = 2.5
f32 = jnp.float32
bf16 = jnp.bfloat16
halo = max(windows)
MIB = 1 << 20
AHEAD = 1 << 35


vmem = pl.BlockSpec(memory_space=pltpu.VMEM)
smem = pl.BlockSpec(memory_space=pltpu.SMEM)


def call(body, outs, n_in, flops, nbytes, limit, scalars=0, scratch=()):
    return pl.pallas_call(
        body,
        out_shape=outs,
        in_specs=[smem] * scalars + [vmem] * n_in,
        out_specs=jax.tree.map(lambda _: vmem, outs),
        scratch_shapes=scratch,
        cost_estimate=pl.CostEstimate(flops=flops, bytes_accessed=nbytes, transcendentals=0),
        compiler_params=pltpu.CompilerParams(vmem_limit_bytes=limit),
    )


def dot(a, b):
    return jnp.dot(a, b, preferred_element_type=f32)


def silu_mul(gate, up):
    return gate / (1.0 + jnp.exp(-gate)) * up


def cut_body(parts, where, pool, *outs):
    rows = pool.shape[0]
    tokens = outs[0].shape[0] - halo
    for j in range(parts):
        start = pl.multiple_of(lax.rem(where[1] + j, parts) * tokens, halo)
        before = pl.multiple_of(lax.rem(start + rows - halo, rows), halo)
        outs[j][:halo, :] = pool[pl.ds(before, halo), :]
        outs[j][halo:, :] = pool[pl.ds(start, tokens), :]
    outs[parts][...] = pool[rows - halo :, :]


def meta_body(ids, scores, meta):
    top = ids.shape[0]
    meta[:top, :] = ids[...].astype(f32)
    meta[top:, :] = scores[...]


def mixer_body(parts, where, *refs):
    mains, halos = refs[:parts], refs[parts : 2 * parts]
    residual, maps, scale, proj, gain, settled_ref, normed_ref, mixed_ref = refs[2 * parts :]
    rows, channels = mains[0].shape[0] - halo, mains[0].shape[1]
    width = maps.shape[1]
    groups_here = channels // width
    place = where[0] * rows + lax.broadcasted_iota(jnp.int32, (rows, width), 0)
    for j in range(parts):
        part = lax.rem(where[1] + parts - j, parts)
        for g in range(groups_here):
            cols = slice(g * width, (g + 1) * width)
            here = mains[j][halo:, cols].astype(f32)
            outer = halos[j][:, cols].astype(f32) * jnp.where(where[0] > 0, 1.0, 0.0)
            before = jnp.where(where[1] > 0, mains[j][:halo, cols].astype(f32), outer)
            total = jnp.concatenate([before, here], axis=0)
            span = 1
            while span < windows[g % 4]:
                total = total + pltpu.roll(total, span, 0)
                span *= 2
            pooled = total[halo:] / jnp.minimum(place + 1, span).astype(f32)
            contrast = (pooled - here).astype(bf16)
            group = part * groups_here + g
            mapped = dot(contrast, maps[group]) * scale[pl.ds(group, 1), :]
            at = pl.multiple_of(group * width, width)
            mixed_ref[:, pl.ds(at, width)] = mapped.astype(bf16)
    model = residual.shape[1]
    step = min(model, 512)
    squares = jnp.zeros((rows, 1), f32)
    for c in range(0, model, step):
        wide = residual[:, c : c + step].astype(f32) + dot(mixed_ref[...], proj[:, c : c + step])
        wide = wide.astype(bf16)
        settled_ref[:, c : c + step] = wide
        wide = wide.astype(f32)
        squares = squares + jnp.sum(wide * wide, axis=1, keepdims=True)
    inverse = lax.rsqrt(squares / model + epsilon)
    for c in range(0, model, step):
        wide = settled_ref[:, c : c + step].astype(f32)
        normed_ref[:, c : c + step] = (wide * inverse * gain[:, c : c + step]).astype(bf16)


def mixer(parts, where, mains, halos, residual, maps, scale, proj, gain):
    rows, model = residual.shape
    out = jax.ShapeDtypeStruct((rows, model), bf16)
    return pl.pallas_call(
        functools.partial(mixer_body, parts),
        out_shape=(out, out),
        in_specs=[smem] + [vmem] * (2 * parts + 5),
        out_specs=(vmem, vmem),
        scratch_shapes=[pltpu.VMEM((rows, proj.shape[0]), bf16)],
        name="mixer",
        cost_estimate=pl.CostEstimate(
            flops=AHEAD, bytes_accessed=AHEAD // 100, transcendentals=0
        ),
        compiler_params=pltpu.CompilerParams(vmem_limit_bytes=8 * MIB),
    )(where, *mains, *halos, residual, maps, scale, proj, gain)


def shared_body(normed, settled, gate, up, down, base_ref):
    hidden = silu_mul(dot(normed[...], gate[...]), dot(normed[...], up[...])).astype(bf16)
    model = base_ref.shape[1]
    step = min(model, 512)
    for c in range(0, model, step):
        base_ref[:, c : c + step] = settled[:, c : c + step].astype(f32) + dot(
            hidden, down[:, c : c + step]
        )


def pack_body(slots, top, where, meta, rows_ref, *outs):
    outs, (high_ref, low_ref) = outs[:-2], outs[-2:]
    count = len(outs)
    tokens = rows_ref.shape[0]
    index = lax.broadcasted_iota(jnp.int32, (count, tokens), 0)
    scores = meta[top : 2 * top, :]
    shares = scores / jnp.sum(scores, axis=0, keepdims=True) * routed_scale
    earlier = lax.broadcasted_iota(jnp.int32, (tokens, tokens), 0) < lax.broadcasted_iota(
        jnp.int32, (tokens, tokens), 1
    )
    earlier = earlier.astype(f32).astype(bf16)
    slot = lax.broadcasted_iota(jnp.int32, (slots, tokens), 0).astype(f32)

    expert = (where[0] + (where[1] ^ index)).astype(f32)
    named = jnp.zeros((count, tokens), f32)
    weight = jnp.zeros((count, tokens), f32)
    for k in range(top):
        hit = meta[k : k + 1, :] == expert
        named = jnp.where(hit, 1.0, named)
        weight = jnp.where(hit, shares[k : k + 1, :], weight)
    position = jnp.where(named > 0, dot(named.astype(bf16), earlier), -1.0)
    picks = [jnp.where(position[j : j + 1] == slot, 1.0, 0.0) for j in range(count)]
    factors = jnp.concatenate([picks[j] * weight[j : j + 1] for j in range(count)], axis=0)
    picks = jnp.concatenate(picks, axis=0).astype(bf16)
    high = factors.astype(bf16)
    high_ref[...] = high
    low_ref[...] = (factors - high.astype(f32)).astype(bf16)
    model = rows_ref.shape[1]
    step = min(model, 512)
    for c in range(0, model, step):
        chosen = dot(picks, rows_ref[:, c : c + step])
        spread(outs, c, chosen)


def pack(count, slots, where, meta, rows):
    tokens, model = rows.shape
    piece = jax.ShapeDtypeStruct((slots, model), bf16)
    factor = jax.ShapeDtypeStruct((count * slots, tokens), bf16)
    out = call(
        functools.partial(pack_body, slots, meta.shape[0] // 2),
        (piece,) * count + (factor,) * 2,
        2,
        AHEAD,
        AHEAD // 100,
        4 * MIB,
        1,
    )(where, meta, rows)
    return out[:count], out[count:]


def spread(outs, c, values):
    rows = outs[0].shape[0]
    for j, out in enumerate(outs):
        part = values[j * rows : (j + 1) * rows]
        out[:, c : c + values.shape[1]] = part.astype(bf16)


def gathered(refs):
    return jnp.concatenate([r[...].astype(f32) for r in refs], axis=0).astype(bf16)


def expert_body(count, *refs):
    pieces, (gate, up, down) = refs[:count], refs[count : count + 3]
    outs, held = refs[count + 3 : -1], refs[-1]
    held[...] = gathered(pieces)
    hidden = silu_mul(dot(held[...], gate[0]), dot(held[...], up[0])).astype(bf16)
    model = held.shape[1]
    step = min(model, 512)
    for c in range(0, model, step):
        spread(outs, c, dot(hidden, down[0, :, c : c + step]))


def expert(pieces, gate, up, down):
    count = len(pieces)
    slots, model = pieces[0].shape
    return call(
        functools.partial(expert_body, count),
        (jax.ShapeDtypeStruct((slots, model), bf16),) * count,
        count + 3,
        6 * count * slots * gate.size,
        6 * gate.size,
        8 * MIB,
        0,
        [pltpu.VMEM((count * slots, model), bf16)],
    )(*pieces, gate, up, down)


def weighted(high, low, rows):
    dims = (((0,), (0,)), ((), ()))
    return lax.dot_general(high, rows, dims, preferred_element_type=f32) + lax.dot_general(
        low, rows, dims, preferred_element_type=f32
    )


def combine_body(count, *refs):
    pieces, (high, low) = refs[:count], refs[count : count + 2]
    earlier, out_ref = refs[count + 2 : -1], refs[-1]
    model = out_ref.shape[1]
    step = min(model, 512)
    for c in range(0, model, step):
        rows = gathered([r.at[:, c : c + step] for r in pieces])
        total = weighted(high[...], low[...], rows)
        for e in earlier:
            total = total + e[:, c : c + step].astype(f32)
        out_ref[:, c : c + step] = total.astype(bf16)


def combine(pieces, factors, earlier):
    count = len(pieces)
    slots, model = pieces[0].shape
    tokens = factors[0].shape[1]
    return call(
        functools.partial(combine_body, count),
        jax.ShapeDtypeStruct((tokens, model), bf16),
        count + 2 + len(earlier),
        4 * count * slots * tokens * model,
        2 * count * slots * model,
        4 * MIB,
    )(*pieces, *factors, *earlier)


def final_body(count, extra, *refs):
    pieces = refs[:count]
    high, low, base = refs[count : count + 3]
    partials = refs[count + 3 : count + 3 + extra]
    out_ref = refs[count + 3 + extra]
    model = out_ref.shape[1]
    step = min(model, 512)
    for c in range(0, model, step):
        cols = slice(c, c + step)
        rows = gathered([r.at[:, cols] for r in pieces])
        total = base[:, cols] + weighted(high[...], low[...], rows)
        for p in partials:
            total = total + p[:, cols].astype(f32)
        out_ref[:, cols] = total.astype(bf16)


def final(pieces, factors, base, partials):
    count = len(pieces)
    return call(
        functools.partial(final_body, count, len(partials)),
        jax.ShapeDtypeStruct(base.shape, bf16),
        count + 3 + len(partials),
        4 * count * pieces[0].shape[0] * base.size,
        4 * base.size,
        4 * MIB,
    )(*pieces, *factors, base, *partials)


def on_device(
    residual,
    pool_input,
    group_maps,
    pool_scale,
    out_proj,
    norm_gain,
    shared_gate,
    shared_up,
    shared_down,
    expert_gate,
    expert_up,
    expert_down,
    expert_ids,
    route_score,
):
    axes = ("sp", "tp")
    size_sp, size_tp = lax.axis_size("sp"), lax.axis_size("tp")
    devices = size_sp * size_tp
    me = lax.axis_index(axes)
    my_tp = lax.axis_index("tp")
    tokens, model = residual.shape
    channels = pool_input.shape[1]
    top = expert_ids.shape[1]
    capacity = 3 * tokens * top // (2 * devices)
    slots = -(-capacity // 8) * 8
    planes = 1
    while size_sp % (2 * planes) == 0 and capacity * devices >= 2 * planes * tokens:
        planes *= 2
    size_plane = devices // planes

    def move(x, target):
        pairs = [(i, target(i)) for i in range(devices)]
        return lax.ppermute(x, axes, [p for p in pairs if p[1] is not None])

    def along(by):
        return lambda i: (i + by * size_plane) % devices

    def inside(j):
        return lambda i: i // size_plane * size_plane + (i % size_plane ^ j)

    def exchange(pieces):
        return [move(p, inside(j)) if j else p for j, p in enumerate(pieces)]

    where = jnp.stack([me, my_tp]).astype(jnp.int32)
    main = jax.ShapeDtypeStruct((tokens + halo, channels), bf16)
    tail = jax.ShapeDtypeStruct((halo, channels), bf16)
    *mains, tail = call(
        functools.partial(cut_body, size_tp),
        (main,) * size_tp + (tail,),
        1,
        AHEAD,
        AHEAD // 100,
        4 * MIB,
        1,
    )(where, pool_input)
    halos = []
    for j in range(size_tp):

        def core(i, j=j):
            return i // size_tp * size_tp + (i + j) % size_tp

        if j:
            mains[j] = move(mains[j], core)
        halos.append(move(tail, lambda i: (core(i) + size_tp) % devices))
    settled, normed = mixer(
        size_tp,
        where,
        mains,
        halos,
        residual,
        group_maps,
        pool_scale.reshape(-1, group_maps.shape[1]),
        out_proj,
        norm_gain.reshape(1, -1),
    )
    base = call(
        shared_body,
        jax.ShapeDtypeStruct((tokens, model), f32),
        5,
        6 * tokens * shared_gate.size,
        6 * shared_gate.size,
        8 * MIB,
    )(normed, settled, shared_gate, shared_up, shared_down)

    mine = lax.rem(me, size_plane)
    spot = jnp.stack([me - mine, mine]).astype(jnp.int32)
    ahead, behind = planes // 2, (planes - 1) // 2
    hops = list(range(ahead + 1)) + list(range(-1, -behind - 1, -1))

    blocks, arrived, factors, results, back = {0: normed}, {}, {}, {}, {}
    for k in hops[1:]:
        one = 1 if k > 0 else -1
        blocks[k] = move(blocks[k - one], along(one))
    ids, scores, _ = lax.optimization_barrier((expert_ids.T, route_score.T, normed))
    meta = call(
        meta_body,
        jax.ShapeDtypeStruct((2 * top, tokens), f32),
        2,
        2 * top * tokens,
        8 * top * tokens,
        2 * MIB,
    )(ids, scores)
    held, span = [meta], 1
    while span < planes:
        near = jnp.concatenate(held, axis=0) if span > 1 else meta
        far = move(near, along(span))
        held += [far[i : i + 2 * top] for i in range(0, far.shape[0], 2 * top)]
        span *= 2
    metas = {k: held[k % planes] for k in hops}
    for k in hops:
        sent, factors[k] = pack(size_plane, slots, spot, metas[k], blocks[k])
        arrived[k] = exchange(sent)
        results[k] = expert(arrived[k], expert_gate, expert_up, expert_down)
        back[k] = exchange(results[k])

    def homeward(chain, by):
        carried = []
        for k in chain:
            total = combine(back[k], factors[k], carried)
            carried = [move(total, along(by))]
        return carried

    partials = homeward(range(ahead - 1, 0, -1), -1)
    partials += homeward([ahead] + list(range(-behind, 0)), 1)
    return final(back[0], factors[0], base, partials)


def solution(mesh):
    lines = P(("sp", "tp"), None)
    stacked = P(("sp", "tp"), None, None)
    in_specs = (
        (lines, P("sp", "tp")) + (P(),) * 7 + (stacked,) * 3 + (lines, lines)
    )

    return jax.shard_map(
        on_device, mesh=mesh, in_specs=in_specs, out_specs=lines, check_vma=False
    )
```
